512 devices in a mesh: grp: 2 (over y), fs: 32 (over z), tp: 8 (over x, core).
Axes of the slice: x: 4, y: 2, z: 32, core: 2. Of those that a mesh axis runs over, the one named last changes fastest.
The devices are a block of a 4x8x32 slice.
Arguments:
- tokens: bfloat16 [24576, 2048], P(('grp', 'fs'), 'tp'), parts along dimension 0, may hold values from -6 to 6
- mix_gain: float32 [2048], replicated, may hold values from 0.1 to 1.9
- w_signal: bfloat16 [2048, 1024], P('fs', 'tp'), may hold values from -0.125 to 0.125
- w_outer_gate: bfloat16 [2048, 1024], P('fs', 'tp'), may hold values from -0.125 to 0.125
- w_inner_gate: bfloat16 [2048, 1024], P('fs', 'tp'), may hold values from -0.125 to 0.125
- mix_taps: float32 [3, 1024], P(None, 'tp'), may hold values from -3 to 3
- w_mix_out: bfloat16 [1024, 2048], P('tp', 'fs'), may hold values from -0.1875 to 0.1875
- ffn_gain: float32 [2048], replicated, may hold values from 0.1 to 1.9
- w_gate: bfloat16 [2048, 5120], P('fs', 'tp'), may hold values from -0.125 to 0.125
- w_value: bfloat16 [2048, 5120], P('fs', 'tp'), may hold values from -0.125 to 0.125
- up_taps: float32 [2, 3, 5120], P(None, None, 'tp'), may hold values from -3 to 3
- up_bias: float32 [2, 5120], P(None, 'tp'), may hold values from -3 to 3
- w_down: bfloat16 [5120, 2048], P('tp', 'fs'), may hold values from -0.078125 to 0.078125
Outputs:
- layer_out: bfloat16 [24576, 2048], P(('grp', 'fs'), 'tp'), parts along dimension 0
The draws below stay inside these ranges and needn't reach their ends.
There are 2 independent parts, one for each index of `grp`. The reference program is written for one: setup_inputs(seed, part) draws one part's arguments, and reference() takes and returns one part's arrays. A program takes and returns all parts, laid end to end along the dimension named above; an argument that names none is the same for every part. Nothing has to cross between parts.
All inputs are finite; a program needn't handle non-finite values.
Results may differ from the reference program's by a relative error of at most 0.022.
Values may be sent and summed in bfloat16 or wider, within the bound.
No kernel may reach another device: no remote copies, remote signals or barrier semaphores. Data moves between devices by JAX's collectives and lax.ppermute only.
A program may use at most 64 MiB of HBM per device.

```python
import jax
import jax.numpy as jnp
from jax import lax

D = 2048
DC = 1024
FF = 5120
TAPS = 3
LEN = 192
TOKENS = 12288
N_TP = 8


def block_levels(stream_key, extent, split, least, high):
    level, own = 1.0, jax.random.fold_in(stream_key, 6)
    for dim, blocks in split:
        steps = jnp.exp(jax.random.uniform(jax.random.fold_in(own, dim), (blocks,), jnp.float32, least / len(split), high / len(split)))
        level = level * jnp.repeat(steps, extent[dim] // blocks).reshape([-1 if axis == dim else 1 for axis in range(len(extent))])
    return level


def centred(rng, dims, deviation, bound, shards=(), dtype=jnp.bfloat16):
    drawn = jax.random.normal(rng, dims, jnp.float32) * deviation
    if len(shards) > 0:
        drawn = block_levels(rng, dims, shards, -0.22, 0.18) * drawn
    return jnp.clip(drawn, min=-bound, max=bound).astype(dtype)


def setup_inputs(seed: int = 0, part: int = 0) -> dict:
    key_list = jax.random.split(jax.random.key(seed), 14)
    part_splits = jax.random.split(jax.random.fold_in(key_list[13], part), 14)
    return {
        "tokens": centred(part_splits[0], (TOKENS, D), 1.0, 6.0, ((0, 32), (1, 8))),
        "mix_gain": jnp.clip(1.0 + 0.18 * jax.random.normal(key_list[1], (D,), jnp.float32), 0.1, 1.9),
        "w_signal": centred(key_list[2], (D, DC), D ** -0.5, 0.125, ((0, 32), (1, 8))),
        "w_outer_gate": centred(key_list[3], (D, DC), D ** -0.5, 0.125, ((0, 32), (1, 8))),
        "w_inner_gate": centred(key_list[4], (D, DC), D ** -0.5, 0.125, ((0, 32), (1, 8))),
        "mix_taps": centred(key_list[5], (TAPS, DC), 0.577, 3.0, ((1, 8),), jnp.float32),
        "w_mix_out": centred(key_list[6], (DC, D), DC ** -0.5, 0.1875, ((0, 8), (1, 32))),
        "ffn_gain": jnp.clip(1.0 + 0.18 * jax.random.normal(key_list[7], (D,), jnp.float32), 0.1, 1.9),
        "w_gate": centred(key_list[8], (D, FF), D ** -0.5, 0.125, ((0, 32), (1, 8))),
        "w_value": centred(key_list[9], (D, FF), D ** -0.5, 0.125, ((0, 32), (1, 8))),
        "up_taps": centred(key_list[10], (2, TAPS, FF), 0.577, 3.0, ((2, 8),), jnp.float32),
        "up_bias": centred(key_list[11], (2, FF), 0.5, 3.0, ((1, 8),), jnp.float32),
        "w_down": centred(key_list[12], (FF, D), FF ** -0.5, 0.078125, ((0, 8), (1, 32))),
    }


def conv_positions(values, taps):
    width = values.shape[1]
    blocks = values.reshape(-1, LEN, width)
    padded = jnp.pad(blocks, ((0, 0), (2, 0), (0, 0)))
    result = padded[:, 0:LEN] * taps[0] + padded[:, 1:LEN + 1] * taps[1] + padded[:, 2:LEN + 2] * taps[2]
    return result.reshape(-1, width)

def rms_norm(stream, gain):
    values = stream.astype(jnp.float32)
    scale = lax.rsqrt(lax.optimization_barrier(jnp.mean(values * values, axis=-1, keepdims=True)) + 1e-06)
    return (values * scale * gain).astype(jnp.bfloat16)

def block_partials(left, right, blocks):
    width = left.shape[1] // blocks
    total = jnp.zeros((left.shape[0], right.shape[1]), jnp.float32)
    for index in range(blocks):
        part = jnp.dot(left[:, index * width:(index + 1) * width], right[index * width:(index + 1) * width], preferred_element_type=jnp.float32)
        part = lax.optimization_barrier(part.astype(jnp.bfloat16))
        total = total + part.astype(jnp.float32)
    return total

def reference(tokens, mix_gain, w_signal, w_outer_gate, w_inner_gate, mix_taps, w_mix_out, ffn_gain, w_gate, w_value, up_taps, up_bias, w_down):
    normed = rms_norm(tokens, mix_gain)
    signal = jnp.dot(normed, w_signal, preferred_element_type=jnp.float32).astype(jnp.bfloat16)
    outer = jnp.dot(normed, w_outer_gate, preferred_element_type=jnp.float32).astype(jnp.bfloat16)
    inner = jnp.dot(normed, w_inner_gate, preferred_element_type=jnp.float32).astype(jnp.bfloat16)
    product = inner.astype(jnp.float32) * signal.astype(jnp.float32)
    mixed = (outer.astype(jnp.float32) * conv_positions(product, mix_taps)).astype(jnp.bfloat16)
    mix_sum = block_partials(mixed, w_mix_out, N_TP)
    resid = (tokens.astype(jnp.float32) + mix_sum).astype(jnp.bfloat16)
    normed_ffn = rms_norm(resid, ffn_gain)
    gate = jnp.dot(normed_ffn, w_gate, preferred_element_type=jnp.float32).astype(jnp.bfloat16)
    value = jnp.dot(normed_ffn, w_value, preferred_element_type=jnp.float32).astype(jnp.bfloat16)
    gate_conv = conv_positions(gate.astype(jnp.float32), up_taps[0]) + up_bias[0]
    value_conv = conv_positions(value.astype(jnp.float32), up_taps[1]) + up_bias[1]
    hidden = (jax.nn.silu(gate_conv) * value_conv).astype(jnp.bfloat16)
    ffn_sum = block_partials(hidden, w_down, N_TP)
    return (resid.astype(jnp.float32) + ffn_sum).astype(jnp.bfloat16)
```

```python
import jax
import jax.numpy as jnp
from jax import lax
from jax.sharding import PartitionSpec as P

SEQS_DEV = 2


def in_one_piece(arrays, axis, dim, along):
    widths = [a.shape[along] for a in arrays]
    both = jnp.concatenate(arrays, axis=along)
    filled = lax.all_gather(both, axis, axis=dim, tiled=True)
    return tuple(jnp.split(filled, [sum(widths[:k]) for k in range(1, len(widths))], axis=along))


def copy_for_each(value, axis):
    copies = jnp.broadcast_to(value, (lax.axis_size(axis), *value.shape))
    return lax.all_to_all(copies, axis, split_axis=0, concat_axis=0, tiled=True)


def in_order(pieces, dim):
    shape = list(pieces.shape[1:])
    shape[dim] *= pieces.shape[0]
    return jnp.moveaxis(pieces, 0, dim).reshape(shape)


def gathered_copies(value, axis, dim):
    pieces = copy_for_each(value, axis)
    return in_order(pieces, dim)


def split_up(value, dim, devices):
    shape = value.shape
    pieces = value.reshape(*shape[:dim], devices, shape[dim] // devices, *shape[dim + 1 :])
    return jnp.moveaxis(pieces, dim, 0)


def sent_and_summed(value, axis, dim):
    devices = lax.axis_size(axis)
    pieces = lax.all_to_all(split_up(value, dim, devices), axis, 0, 0, tiled=True)
    return jnp.sum(pieces.astype(jnp.float32), axis=0)


def conv_positions(values, taps):
    width = values.shape[1]
    blocks = values.reshape(SEQS_DEV, -1, width)
    length = blocks.shape[1]
    padded = jnp.pad(blocks, ((0, 0), (2, 0), (0, 0)))
    result = (
        padded[:, 0:length] * taps[0]
        + padded[:, 1 : length + 1] * taps[1]
        + padded[:, 2 : length + 2] * taps[2]
    )
    return result.reshape(-1, width)


def rms_norm(stream, gain):
    values = stream.astype(jnp.float32)
    scale = lax.rsqrt(jnp.mean(values * values, axis=-1, keepdims=True) + 1e-06)
    return (values * scale * gain).astype(jnp.bfloat16)


def dot_t(left, right_t):
    return lax.dot_general(
        left, right_t, (((1,), (1,)), ((), ())), preferred_element_type=jnp.float32
    )


def on_device(
    tokens,
    mix_gain,
    w_signal,
    w_outer_gate,
    w_inner_gate,
    mix_taps,
    w_mix_out,
    ffn_gain,
    w_gate,
    w_value,
    up_taps,
    up_bias,
    w_down,
):
    shards = (w_signal, w_outer_gate, w_inner_gate, w_mix_out.T, w_gate, w_value, w_down.T)
    (
        signal_full,
        outer_full,
        inner_full,
        mix_out_t,
        gate_full,
        value_full,
        down_t,
    ) = in_one_piece(shards, "fs", 0, 1)
    whole = gathered_copies(tokens, "tp", 1)
    normed = rms_norm(whole, mix_gain)
    signal = jnp.dot(normed, signal_full, preferred_element_type=jnp.float32)
    outer = jnp.dot(normed, outer_full, preferred_element_type=jnp.float32)
    inner = jnp.dot(normed, inner_full, preferred_element_type=jnp.float32)
    signal = signal.astype(jnp.bfloat16).astype(jnp.float32)
    outer = outer.astype(jnp.bfloat16).astype(jnp.float32)
    inner = inner.astype(jnp.bfloat16).astype(jnp.float32)
    mixed = (outer * conv_positions(inner * signal, mix_taps)).astype(jnp.bfloat16)
    mix_terms = dot_t(mixed, mix_out_t)
    mix_sum = sent_and_summed(mix_terms.astype(jnp.bfloat16), "tp", 1)
    resid = (tokens.astype(jnp.float32) + mix_sum).astype(jnp.bfloat16)
    whole_ffn = gathered_copies(resid, "tp", 1)
    normed_ffn = rms_norm(whole_ffn, ffn_gain)
    gate = jnp.dot(normed_ffn, gate_full, preferred_element_type=jnp.float32)
    value = jnp.dot(normed_ffn, value_full, preferred_element_type=jnp.float32)
    gate = gate.astype(jnp.bfloat16).astype(jnp.float32)
    value = value.astype(jnp.bfloat16).astype(jnp.float32)
    gate_conv = conv_positions(gate, up_taps[0]) + up_bias[0]
    value_conv = conv_positions(value, up_taps[1]) + up_bias[1]
    hidden = (jax.nn.silu(gate_conv) * value_conv).astype(jnp.bfloat16)
    ffn_terms = dot_t(hidden, down_t)
    ffn_sum = sent_and_summed(ffn_terms.astype(jnp.bfloat16), "tp", 1)
    return (resid.astype(jnp.float32) + ffn_sum).astype(jnp.bfloat16)


def solution(mesh):
    placed = (
        P(("grp", "fs"), "tp"),
        P(),
        P("fs", "tp"),
        P("fs", "tp"),
        P("fs", "tp"),
        P(None, "tp"),
        P("tp", "fs"),
        P(),
        P("fs", "tp"),
        P("fs", "tp"),
        P(None, None, "tp"),
        P(None, "tp"),
        P("tp", "fs"),
    )
    return jax.shard_map(
        on_device, mesh=mesh, in_specs=placed, out_specs=P(("grp", "fs"), "tp"), check_vma=False
    )
```

```python
import jax
import jax.numpy as jnp
from jax import lax
from jax.sharding import Mesh
from jax.sharding import PartitionSpec as P

SEQS_DEV = 2
CORES = 2
NEAR = 4

TP = ("tx", "tc")
FS = ("fa", "fb")


def side_by_side(arrays):
    return jnp.concatenate(arrays, axis=1)


def gathered_copies(value, axis):
    count = lax.axis_size(axis)
    copies = jnp.broadcast_to(value, (count, *value.shape))
    pieces = lax.all_to_all(copies, axis, split_axis=0, concat_axis=0, tiled=True)
    rows, width = value.shape
    return jnp.moveaxis(pieces, 0, 1).reshape(rows, count * width)


def swapped(value, axis):
    return lax.ppermute(value, axis, [(0, 1), (1, 0)])


def by_core(own, other):
    first = lax.axis_index("tc") == 0
    return jnp.where(first, own, other), jnp.where(first, other, own)


def gathered_features(value):
    own = lax.all_gather(value, "tx", axis=0)
    other = swapped(own, "tc")
    pieces = [piece for chip in range(own.shape[0]) for piece in by_core(own[chip], other[chip])]
    return jnp.concatenate(pieces, axis=1)


def sent_and_summed(terms):
    chips = lax.axis_size("tx")
    width = terms.shape[1] // (chips * CORES)
    blocks = [terms[:, k * width : (k + 1) * width] for k in range(chips * CORES)]
    chosen = [by_core(*blocks[k : k + CORES]) for k in range(0, chips * CORES, CORES)]
    keep = jnp.stack([pair[0] for pair in chosen])
    send = jnp.stack([pair[1] for pair in chosen])
    received = swapped(send.astype(jnp.bfloat16), "tc")
    pairs = (keep + received.astype(jnp.float32)).astype(jnp.bfloat16)
    parts = lax.all_to_all(pairs, "tx", 0, 0, tiled=True)
    return jnp.sum(parts.astype(jnp.float32), axis=0)


def conv_positions(values, taps):
    width = values.shape[1]
    blocks = values.reshape(SEQS_DEV, -1, width)
    length = blocks.shape[1]
    padded = jnp.pad(blocks, ((0, 0), (2, 0), (0, 0)))
    result = (
        padded[:, 0:length] * taps[0]
        + padded[:, 1 : length + 1] * taps[1]
        + padded[:, 2 : length + 2] * taps[2]
    )
    return result.reshape(-1, width)


def rms_norm(stream, gain):
    values = stream.astype(jnp.float32)
    scale = lax.rsqrt(jnp.mean(values * values, axis=-1, keepdims=True) + 1e-06)
    return (values * scale * gain).astype(jnp.bfloat16)


def dot(left, right):
    return jnp.dot(left, right, preferred_element_type=jnp.float32)


def dot_t(left, right_t):
    return lax.dot_general(
        left, right_t, (((1,), (1,)), ((), ())), preferred_element_type=jnp.float32
    )


def near_gather(far):
    wide = lax.all_gather(far, "fb", axis=1, tiled=True)
    return wide.reshape(-1, far.shape[-1])


def rounded(value):
    return value.astype(jnp.bfloat16).astype(jnp.float32)


def mixer_weights(w_signal, w_outer_gate, w_inner_gate, mix_out_t, paired):
    if not paired:
        shards = (w_signal, w_inner_gate, w_outer_gate, mix_out_t)
        far = lax.all_gather(side_by_side(shards), "fa", axis=0)
        width = w_signal.shape[1]
        return tuple(near_gather(far[:, :, k * width : (k + 1) * width]) for k in range(4))
    first = lax.axis_index("pair") == 0
    early = jnp.where(first, w_signal, w_inner_gate)
    late = jnp.where(first, w_outer_gate, mix_out_t)
    width = early.shape[1]
    far = lax.all_gather(side_by_side((early, late)), "fa", axis=0)
    early_own = near_gather(far[:, :, :width])
    early_other = swapped(early_own, "pair")
    late_own = near_gather(far[:, :, width:])
    late_other = swapped(late_own, "pair")
    outer_full = jnp.where(first, late_own, late_other)
    mix_full = jnp.where(first, late_other, late_own)
    return early_own, early_other, outer_full, mix_full


def on_device(
    tokens,
    mix_gain,
    w_signal,
    w_outer_gate,
    w_inner_gate,
    mix_taps,
    w_mix_out,
    ffn_gain,
    w_gate,
    w_value,
    up_taps,
    up_bias,
    w_down,
    paired,
):
    hidden_width = w_gate.shape[1]
    ffn_full = lax.all_gather(side_by_side((w_gate, w_value, w_down.T)), FS, axis=0, tiled=True)
    whole = gathered_copies(tokens, TP)
    early_a, early_b, outer_full, mix_full = mixer_weights(
        w_signal, w_outer_gate, w_inner_gate, w_mix_out.T, paired
    )
    normed = rms_norm(whole, mix_gain)
    product = rounded(dot(normed, early_a)) * rounded(dot(normed, early_b))
    outer = rounded(dot(normed, outer_full))
    mixed = (outer * conv_positions(product, mix_taps)).astype(jnp.bfloat16)
    mix_sum = sent_and_summed(dot_t(mixed, mix_full))
    resid = (tokens.astype(jnp.float32) + mix_sum).astype(jnp.bfloat16)
    whole_ffn = gathered_features(resid)
    normed_ffn = rms_norm(whole_ffn, ffn_gain)
    gate = rounded(dot(normed_ffn, ffn_full[:, :hidden_width]))
    value = rounded(dot(normed_ffn, ffn_full[:, hidden_width : 2 * hidden_width]))
    gate_conv = conv_positions(gate, up_taps[0]) + up_bias[0]
    value_conv = conv_positions(value, up_taps[1]) + up_bias[1]
    hidden = (jax.nn.silu(gate_conv) * value_conv).astype(jnp.bfloat16)
    ffn_sum = sent_and_summed(dot_t(hidden, ffn_full[:, 2 * hidden_width :]))
    return (resid.astype(jnp.float32) + ffn_sum).astype(jnp.bfloat16)


def solution(mesh):
    groups, depth, wide = (mesh.shape[name] for name in ("grp", "fs", "tp"))
    pair = 2 if groups % 2 == 0 else 1
    split = Mesh(
        mesh.devices.reshape(
            groups // pair, pair, depth // NEAR, NEAR, wide // CORES, CORES
        ),
        ("gp", "pair", *FS, *TP),
    )
    streams = P(("gp", "pair", *FS), TP)
    placed = (
        streams,
        P(),
        P(FS, TP),
        P(FS, TP),
        P(FS, TP),
        P(None, TP),
        P(TP, FS),
        P(),
        P(FS, TP),
        P(FS, TP),
        P(None, None, TP),
        P(None, TP),
        P(TP, FS),
    )

    def body(*args):
        return on_device(*args, paired=pair == 2)

    return jax.shard_map(
        body, mesh=split, in_specs=placed, out_specs=streams, check_vma=False
    )
```

```python
import jax
import jax.numpy as jnp
from jax import lax
from jax.experimental import pallas as pl
from jax.experimental.pallas import tpu as pltpu
from jax.sharding import Mesh
from jax.sharding import PartitionSpec as P

SEQS_DEV = 2
CORES = 2
NEAR = 4

TP = ("tx", "tc")
FS = ("fa", "fb")


def side_by_side(arrays):
    return jnp.concatenate(arrays, axis=1)


def gathered_copies(value, axis):
    count = lax.axis_size(axis)
    copies = jnp.broadcast_to(value, (count, *value.shape))
    pieces = lax.all_to_all(copies, axis, split_axis=0, concat_axis=0, tiled=True)
    rows, width = value.shape
    return jnp.moveaxis(pieces, 0, 1).reshape(rows, count * width)


def swapped(value, axis):
    return lax.ppermute(value, axis, [(0, 1), (1, 0)])


def by_core(own, other):
    first = lax.axis_index("tc") == 0
    return jnp.where(first, own, other), jnp.where(first, other, own)


def gathered_features(value):
    own = lax.all_gather(value, "tx", axis=0)
    other = swapped(own, "tc")
    pieces = [piece for chip in range(own.shape[0]) for piece in by_core(own[chip], other[chip])]
    return jnp.concatenate(pieces, axis=1)


def pairs_and_summed(keep, send):
    received = swapped(send, "tc")
    pairs = (keep.astype(jnp.float32) + received.astype(jnp.float32)).astype(jnp.bfloat16)
    parts = lax.all_to_all(pairs, "tx", 0, 0, tiled=True)
    return jnp.sum(parts.astype(jnp.float32), axis=0)


def sent_and_summed(terms):
    chips = lax.axis_size("tx")
    width = terms.shape[1] // (chips * CORES)
    blocks = [terms[:, k * width : (k + 1) * width] for k in range(chips * CORES)]
    chosen = [by_core(*blocks[k : k + CORES]) for k in range(0, chips * CORES, CORES)]
    keep = jnp.stack([pair[0] for pair in chosen])
    send = jnp.stack([pair[1] for pair in chosen])
    return pairs_and_summed(keep, send.astype(jnp.bfloat16))


def conv_positions(values, taps):
    width = values.shape[1]
    blocks = values.reshape(SEQS_DEV, -1, width)
    length = blocks.shape[1]
    padded = jnp.pad(blocks, ((0, 0), (2, 0), (0, 0)))
    result = (
        padded[:, 0:length] * taps[0]
        + padded[:, 1 : length + 1] * taps[1]
        + padded[:, 2 : length + 2] * taps[2]
    )
    return result.reshape(-1, width)


def rms_norm(stream, gain):
    values = stream.astype(jnp.float32)
    scale = lax.rsqrt(jnp.mean(values * values, axis=-1, keepdims=True) + 1e-06)
    return (values * scale * gain).astype(jnp.bfloat16)


def dot(left, right):
    return jnp.dot(left, right, preferred_element_type=jnp.float32)


def dot_t(left, right_t):
    return lax.dot_general(
        left, right_t, (((1,), (1,)), ((), ())), preferred_element_type=jnp.float32
    )


LANES = 128


def ffn_body(core, normed, taps, bias, weights, keep, send, up, down, hidden, sems):
    rows, features = normed.shape
    wide = hidden.shape[1]
    blocks = wide // LANES
    chips, _, share = keep.shape

    def up_copy(block, half):
        start = half * wide + block * LANES
        return pltpu.make_async_copy(
            weights.at[:, start : start + LANES],
            up.at[block, :, half * LANES : (half + 1) * LANES],
            sems.at[2 * block + half],
        )

    def down_copy(part):
        piece = pl.ds(part * share, share)
        return pltpu.make_async_copy(
            weights.at[piece, 2 * wide : 3 * wide], down.at[piece], sems.at[2 * blocks + part]
        )

    for block in range(blocks):
        up_copy(block, 0).start()
        up_copy(block, 1).start()
    for part in range(CORES * chips):
        down_copy(part).start()

    length = rows // SEQS_DEV
    place = lax.broadcasted_iota(jnp.int32, (rows, LANES), 0) % length

    def conv(values, half, block):
        cols = slice(block * LANES, (block + 1) * LANES)
        values = values.astype(jnp.bfloat16).astype(jnp.float32)
        one = jnp.where(place >= 1, pltpu.roll(values, 1, 0), 0.0)
        two = jnp.where(place >= 2, pltpu.roll(values, 2, 0), 0.0)
        summed = (
            two * taps[half, 0:1, cols] + one * taps[half, 1:2, cols] + values * taps[half, 2:3, cols]
        )
        return summed + bias[half : half + 1, cols]

    for block in range(blocks):
        up_copy(block, 0).wait()
        up_copy(block, 1).wait()
        both = jnp.dot(normed[...], up[block], preferred_element_type=jnp.float32)
        gate = conv(both[:, :LANES], 0, block)
        value = conv(both[:, LANES:], 1, block)
        act = gate / (1.0 + jnp.exp(-gate))
        hidden[:, block * LANES : (block + 1) * LANES] = (act * value).astype(jnp.bfloat16)

    for part in range(CORES * chips):
        down_copy(part).wait()

    def terms(chip, side):
        piece = pl.ds(pl.multiple_of((CORES * chip + side) * share, share), share)
        return lax.dot_general(
            hidden[...], down[piece], (((1,), (1,)), ((), ())), preferred_element_type=jnp.float32
        )

    own = core[0]
    for chip in range(chips):
        send[chip] = terms(chip, 1 - own).astype(send.dtype)
    for chip in range(chips):
        keep[chip] = terms(chip, own).astype(keep.dtype)


def ffn_terms(normed, taps, bias, weights):
    rows, features = normed.shape
    wide = bias.shape[1]
    chips = lax.axis_size("tx")
    share = features // (chips * CORES)
    blocks = wide // LANES
    vmem = pl.BlockSpec(memory_space=pltpu.VMEM)
    return pl.pallas_call(
        ffn_body,
        in_specs=[
            pl.BlockSpec(memory_space=pltpu.SMEM),
            vmem,
            vmem,
            vmem,
            pl.BlockSpec(memory_space=pltpu.HBM),
        ],
        out_specs=[vmem, vmem],
        out_shape=[
            jax.ShapeDtypeStruct((chips, rows, share), jnp.float32),
            jax.ShapeDtypeStruct((chips, rows, share), jnp.bfloat16),
        ],
        scratch_shapes=[
            pltpu.VMEM((blocks, features, 2 * LANES), jnp.bfloat16),
            pltpu.VMEM((features, wide), jnp.bfloat16),
            pltpu.VMEM((rows, wide), jnp.bfloat16),
            pltpu.SemaphoreType.DMA((2 * blocks + CORES * chips,)),
        ],
        compiler_params=pltpu.CompilerParams(vmem_limit_bytes=24 * 1024 * 1024),
        cost_estimate=pl.CostEstimate(
            flops=2 * rows * features * 3 * wide,
            bytes_accessed=2 * features * 3 * wide + 2 * rows * features,
            transcendentals=rows * wide,
        ),
        name="ffn_terms",
    )(lax.axis_index("tc").astype(jnp.int32).reshape(1), normed, taps, bias, pltpu.with_memory_space_constraint(weights, pltpu.HBM))


def near_gather(far):
    wide = lax.all_gather(far, "fb", axis=1, tiled=True)
    return wide.reshape(-1, far.shape[-1])


def rounded(value):
    return value.astype(jnp.bfloat16).astype(jnp.float32)


def mixer_weights(w_signal, w_outer_gate, w_inner_gate, mix_out_t, paired):
    if not paired:
        shards = (w_signal, w_inner_gate, w_outer_gate, mix_out_t)
        far = lax.all_gather(side_by_side(shards), "fa", axis=0)
        width = w_signal.shape[1]
        return tuple(near_gather(far[:, :, k * width : (k + 1) * width]) for k in range(4))
    first = lax.axis_index("pair") == 0
    early = jnp.where(first, w_signal, w_inner_gate)
    late = jnp.where(first, w_outer_gate, mix_out_t)
    width = early.shape[1]
    far = lax.all_gather(side_by_side((early, late)), "fa", axis=0)
    early_own = near_gather(far[:, :, :width])
    early_other = swapped(early_own, "pair")
    late_own = near_gather(far[:, :, width:])
    late_other = swapped(late_own, "pair")
    outer_full = jnp.where(first, late_own, late_other)
    mix_full = jnp.where(first, late_other, late_own)
    return early_own, early_other, outer_full, mix_full


def on_device(
    tokens,
    mix_gain,
    w_signal,
    w_outer_gate,
    w_inner_gate,
    mix_taps,
    w_mix_out,
    ffn_gain,
    w_gate,
    w_value,
    up_taps,
    up_bias,
    w_down,
    paired,
):
    ffn_full = lax.all_gather(side_by_side((w_gate, w_value, w_down.T)), FS, axis=0, tiled=True)
    whole = gathered_copies(tokens, TP)
    early_a, early_b, outer_full, mix_full = mixer_weights(
        w_signal, w_outer_gate, w_inner_gate, w_mix_out.T, paired
    )
    normed = rms_norm(whole, mix_gain)
    product = rounded(dot(normed, early_a)) * rounded(dot(normed, early_b))
    outer = rounded(dot(normed, outer_full))
    mixed = (outer * conv_positions(product, mix_taps)).astype(jnp.bfloat16)
    mix_sum = sent_and_summed(dot_t(mixed, mix_full))
    resid = (tokens.astype(jnp.float32) + mix_sum).astype(jnp.bfloat16)
    whole_ffn = gathered_features(resid)
    normed_ffn = rms_norm(whole_ffn, ffn_gain)
    ffn_sum = pairs_and_summed(*ffn_terms(normed_ffn, up_taps, up_bias, ffn_full))
    return (resid.astype(jnp.float32) + ffn_sum).astype(jnp.bfloat16)


def solution(mesh):
    groups, depth, wide = (mesh.shape[name] for name in ("grp", "fs", "tp"))
    pair = 2 if groups % 2 == 0 else 1
    split = Mesh(
        mesh.devices.reshape(
            groups // pair, pair, depth // NEAR, NEAR, wide // CORES, CORES
        ),
        ("gp", "pair", *FS, *TP),
    )
    streams = P(("gp", "pair", *FS), TP)
    placed = (
        streams,
        P(),
        P(FS, TP),
        P(FS, TP),
        P(FS, TP),
        P(None, TP),
        P(TP, FS),
        P(),
        P(FS, TP),
        P(FS, TP),
        P(None, None, TP),
        P(None, TP),
        P(TP, FS),
    )

    def body(*args):
        return on_device(*args, paired=pair == 2)

    return jax.shard_map(
        body, mesh=split, in_specs=placed, out_specs=streams, check_vma=False
    )
```

```python
import jax
import jax.numpy as jnp
from jax import lax
from jax.experimental import pallas as pl
from jax.experimental.pallas import tpu as pltpu
from jax.sharding import Mesh
from jax.sharding import PartitionSpec as P

SEQS_DEV = 2
CORES = 2
NEAR = 4

TP = ("tx", "tc")
FS = ("fa", "fb")


def side_by_side(arrays):
    return jnp.concatenate(arrays, axis=1)


def gathered_copies(value, axis):
    count = lax.axis_size(axis)
    copies = jnp.broadcast_to(value, (count, *value.shape))
    pieces = lax.all_to_all(copies, axis, split_axis=0, concat_axis=0, tiled=True)
    rows, width = value.shape
    return jnp.moveaxis(pieces, 0, 1).reshape(rows, count * width)


def swapped(value, axis):
    return lax.ppermute(value, axis, [(0, 1), (1, 0)])


def by_core(own, other):
    first = lax.axis_index("tc") == 0
    return jnp.where(first, own, other), jnp.where(first, other, own)


def gathered_features(value):
    own = lax.all_gather(value, "tx", axis=0)
    other = swapped(own, "tc")
    pieces = [piece for chip in range(own.shape[0]) for piece in by_core(own[chip], other[chip])]
    return jnp.concatenate(pieces, axis=1)


def pairs_and_summed(keep, send):
    received = swapped(send, "tc")
    pairs = (keep + received.astype(jnp.float32)).astype(jnp.bfloat16)
    parts = lax.all_to_all(pairs, "tx", 0, 0, tiled=True)
    return jnp.sum(parts.astype(jnp.float32), axis=0)


def sent_and_summed(terms):
    chips = lax.axis_size("tx")
    width = terms.shape[1] // (chips * CORES)
    blocks = [terms[:, k * width : (k + 1) * width] for k in range(chips * CORES)]
    chosen = [by_core(*blocks[k : k + CORES]) for k in range(0, chips * CORES, CORES)]
    keep = jnp.stack([pair[0] for pair in chosen])
    send = jnp.stack([pair[1] for pair in chosen])
    return pairs_and_summed(keep, send.astype(jnp.bfloat16))


def conv_positions(values, taps):
    width = values.shape[1]
    blocks = values.reshape(SEQS_DEV, -1, width)
    length = blocks.shape[1]
    padded = jnp.pad(blocks, ((0, 0), (2, 0), (0, 0)))
    result = (
        padded[:, 0:length] * taps[0]
        + padded[:, 1 : length + 1] * taps[1]
        + padded[:, 2 : length + 2] * taps[2]
    )
    return result.reshape(-1, width)


def rms_norm(stream, gain):
    values = stream.astype(jnp.float32)
    scale = lax.rsqrt(jnp.mean(values * values, axis=-1, keepdims=True) + 1e-06)
    return (values * scale * gain).astype(jnp.bfloat16)


def dot(left, right):
    return jnp.dot(left, right, preferred_element_type=jnp.float32)


def dot_t(left, right_t):
    return lax.dot_general(
        left, right_t, (((1,), (1,)), ((), ())), preferred_element_type=jnp.float32
    )


def near_gather(far):
    wide = lax.all_gather(far, "fb", axis=1, tiled=True)
    return wide.reshape(-1, far.shape[-1])


def rounded(value):
    return value.astype(jnp.bfloat16).astype(jnp.float32)


def mixer_weights(w_signal, w_outer_gate, w_inner_gate, mix_out_t, paired):
    if not paired:
        shards = (w_signal, w_inner_gate, w_outer_gate, mix_out_t)
        far = lax.all_gather(side_by_side(shards), "fa", axis=0)
        width = w_signal.shape[1]
        return tuple(near_gather(far[:, :, k * width : (k + 1) * width]) for k in range(4))
    first = lax.axis_index("pair") == 0
    early = jnp.where(first, w_signal, w_inner_gate)
    late = jnp.where(first, w_outer_gate, mix_out_t)
    width = early.shape[1]
    far = lax.all_gather(side_by_side((early, late)), "fa", axis=0)
    early_own = near_gather(far[:, :, :width])
    early_other = swapped(early_own, "pair")
    late_own = near_gather(far[:, :, width:])
    late_other = swapped(late_own, "pair")
    return early_own, early_other, late_own, late_other


def mixer_body(where, normed, product, taps, late_a, late_b, keep, send):
    rows = normed.shape[0]
    chips, _, share = keep.shape
    first = where[0] == 0
    own = where[1]
    outer_full = jnp.where(first, late_a[...], late_b[...])
    outer = rounded(dot(normed[...], outer_full))
    values = product[...]
    place = lax.broadcasted_iota(jnp.int32, values.shape, 0) % (rows // SEQS_DEV)
    one = jnp.where(place >= 1, pltpu.roll(values, 1, 0), 0.0)
    two = jnp.where(place >= 2, pltpu.roll(values, 2, 0), 0.0)
    conv = two * taps[0:1, :] + one * taps[1:2, :] + values * taps[2:3, :]
    mixed = (outer * conv).astype(jnp.bfloat16)

    def terms(chip, side):
        piece = pl.ds(pl.multiple_of((CORES * chip + side) * share, share), share)
        return dot_t(mixed, jnp.where(first, late_b[piece, :], late_a[piece, :]))

    for chip in range(chips):
        send[chip] = terms(chip, 1 - own).astype(send.dtype)
    for chip in range(chips):
        keep[chip] = terms(chip, own)


def mixer_terms(normed, product, taps, late_a, late_b, paired):
    rows, features = normed.shape
    width = product.shape[1]
    chips = lax.axis_size("tx")
    share = features // (chips * CORES)
    pair = lax.axis_index("pair") if paired else 0 * lax.axis_index("tc")
    where = jnp.stack([pair, lax.axis_index("tc")]).astype(jnp.int32)
    vmem = pl.BlockSpec(memory_space=pltpu.VMEM)
    return pl.pallas_call(
        mixer_body,
        in_specs=[pl.BlockSpec(memory_space=pltpu.SMEM), vmem, vmem, vmem, vmem, vmem],
        out_specs=[vmem, vmem],
        out_shape=[
            jax.ShapeDtypeStruct((chips, rows, share), jnp.float32),
            jax.ShapeDtypeStruct((chips, rows, share), jnp.bfloat16),
        ],
        compiler_params=pltpu.CompilerParams(vmem_limit_bytes=16 * 1024 * 1024),
        cost_estimate=pl.CostEstimate(
            flops=4 * rows * features * width,
            bytes_accessed=2 * features * (rows + 2 * width) + 6 * rows * features,
            transcendentals=0,
        ),
        name="mixer_terms",
    )(where, normed, product, taps, late_a, late_b)


def on_device(
    tokens,
    mix_gain,
    w_signal,
    w_outer_gate,
    w_inner_gate,
    mix_taps,
    w_mix_out,
    ffn_gain,
    w_gate,
    w_value,
    up_taps,
    up_bias,
    w_down,
    paired,
):
    shards = jnp.stack((w_gate, w_value, w_down.T))
    gate_full, value_full, down_t = lax.all_gather(shards, FS, axis=1, tiled=True)
    whole = gathered_copies(tokens, TP)
    early_a, early_b, late_a, late_b = mixer_weights(
        w_signal, w_outer_gate, w_inner_gate, w_mix_out.T, paired
    )
    normed = rms_norm(whole, mix_gain)
    product = rounded(dot(normed, early_a)) * rounded(dot(normed, early_b))
    mix_sum = pairs_and_summed(
        *mixer_terms(normed, product, mix_taps, late_a, late_b, paired)
    )
    resid = (tokens.astype(jnp.float32) + mix_sum).astype(jnp.bfloat16)
    whole_ffn = gathered_features(resid)
    normed_ffn = rms_norm(whole_ffn, ffn_gain)
    gate = rounded(dot(normed_ffn, gate_full))
    value = rounded(dot(normed_ffn, value_full))
    gate_conv = conv_positions(gate, up_taps[0]) + up_bias[0]
    value_conv = conv_positions(value, up_taps[1]) + up_bias[1]
    hidden = (jax.nn.silu(gate_conv) * value_conv).astype(jnp.bfloat16)
    ffn_sum = sent_and_summed(dot_t(hidden, down_t))
    return (resid.astype(jnp.float32) + ffn_sum).astype(jnp.bfloat16)


def solution(mesh):
    groups, depth, wide = (mesh.shape[name] for name in ("grp", "fs", "tp"))
    pair = 2 if groups % 2 == 0 else 1
    split = Mesh(
        mesh.devices.reshape(
            groups // pair, pair, depth // NEAR, NEAR, wide // CORES, CORES
        ),
        ("gp", "pair", *FS, *TP),
    )
    streams = P(("gp", "pair", *FS), TP)
    placed = (
        streams,
        P(),
        P(FS, TP),
        P(FS, TP),
        P(FS, TP),
        P(None, TP),
        P(TP, FS),
        P(),
        P(FS, TP),
        P(FS, TP),
        P(None, None, TP),
        P(None, TP),
        P(TP, FS),
    )

    def body(*args):
        return on_device(*args, paired=pair == 2)

    return jax.shard_map(
        body, mesh=split, in_specs=placed, out_specs=streams, check_vma=False
    )
```

```python
import jax
import jax.numpy as jnp
from jax import lax
from jax.experimental import pallas as pl
from jax.experimental.pallas import tpu as pltpu
from jax.sharding import Mesh
from jax.sharding import PartitionSpec as P

SEQS_DEV = 2
CORES = 2
NEAR = 4

TP = ("tx", "tc")
FS = ("fa", "fb")


def side_by_side(arrays):
    return jnp.concatenate(arrays, axis=1)


def gathered_copies(value, axis):
    count = lax.axis_size(axis)
    copies = jnp.broadcast_to(value, (count, *value.shape))
    pieces = lax.all_to_all(copies, axis, split_axis=0, concat_axis=0, tiled=True)
    rows, width = value.shape
    return jnp.moveaxis(pieces, 0, 1).reshape(rows, count * width)


def swapped(value, axis):
    return lax.ppermute(value, axis, [(0, 1), (1, 0)])


def by_core(own, other):
    first = lax.axis_index("tc") == 0
    return jnp.where(first, own, other), jnp.where(first, other, own)


def gathered_features(value):
    own = lax.all_gather(value, "tx", axis=0)
    other = swapped(own, "tc")
    pieces = [piece for chip in range(own.shape[0]) for piece in by_core(own[chip], other[chip])]
    return jnp.concatenate(pieces, axis=1)


def pairs_and_summed(keep, send):
    received = swapped(send, "tc")
    pairs = (keep + received.astype(jnp.float32)).astype(jnp.bfloat16)
    parts = lax.all_to_all(pairs, "tx", 0, 0, tiled=True)
    return jnp.sum(parts.astype(jnp.float32), axis=0)


def conv_positions(values, taps):
    width = values.shape[1]
    blocks = values.reshape(SEQS_DEV, -1, width)
    length = blocks.shape[1]
    padded = jnp.pad(blocks, ((0, 0), (2, 0), (0, 0)))
    result = (
        padded[:, 0:length] * taps[0]
        + padded[:, 1 : length + 1] * taps[1]
        + padded[:, 2 : length + 2] * taps[2]
    )
    return result.reshape(-1, width)


def rms_norm(stream, gain):
    values = stream.astype(jnp.float32)
    scale = lax.rsqrt(jnp.mean(values * values, axis=-1, keepdims=True) + 1e-06)
    return (values * scale * gain).astype(jnp.bfloat16)


def dot(left, right):
    return jnp.dot(left, right, preferred_element_type=jnp.float32)


def dot_t(left, right_t):
    return lax.dot_general(
        left, right_t, (((1,), (1,)), ((), ())), preferred_element_type=jnp.float32
    )


def near_gather(far):
    wide = lax.all_gather(far, "fb", axis=1, tiled=True)
    return wide.reshape(-1, far.shape[-1])


def rounded(value):
    return value.astype(jnp.bfloat16).astype(jnp.float32)


def mixer_weights(w_signal, w_outer_gate, w_inner_gate, mix_out_t, paired):
    if not paired:
        shards = (w_signal, w_inner_gate, w_outer_gate, mix_out_t)
        far = lax.all_gather(side_by_side(shards), "fa", axis=0)
        width = w_signal.shape[1]
        return tuple(near_gather(far[:, :, k * width : (k + 1) * width]) for k in range(4))
    first = lax.axis_index("pair") == 0
    early = jnp.where(first, w_signal, w_inner_gate)
    late = jnp.where(first, w_outer_gate, mix_out_t)
    width = early.shape[1]
    far = lax.all_gather(side_by_side((early, late)), "fa", axis=0)
    early_own = near_gather(far[:, :, :width])
    early_other = swapped(early_own, "pair")
    late_own = near_gather(far[:, :, width:])
    late_other = swapped(late_own, "pair")
    return early_own, early_other, late_own, late_other


def mixer_body(where, normed, product, taps, late_a, late_b, keep, send):
    rows = normed.shape[0]
    chips, _, share = keep.shape
    first = where[0] == 0
    own = where[1]
    outer_full = jnp.where(first, late_a[...], late_b[...])
    outer = rounded(dot(normed[...], outer_full))
    values = product[...]
    place = lax.broadcasted_iota(jnp.int32, values.shape, 0) % (rows // SEQS_DEV)
    one = jnp.where(place >= 1, pltpu.roll(values, 1, 0), 0.0)
    two = jnp.where(place >= 2, pltpu.roll(values, 2, 0), 0.0)
    conv = two * taps[0:1, :] + one * taps[1:2, :] + values * taps[2:3, :]
    mixed = (outer * conv).astype(jnp.bfloat16)

    def terms(chip, side):
        piece = pl.ds(pl.multiple_of((CORES * chip + side) * share, share), share)
        return dot_t(mixed, jnp.where(first, late_b[piece, :], late_a[piece, :]))

    for chip in range(chips):
        send[chip] = terms(chip, 1 - own).astype(send.dtype)
    for chip in range(chips):
        keep[chip] = terms(chip, own)


def mixer_terms(normed, product, taps, late_a, late_b, paired):
    rows, features = normed.shape
    width = product.shape[1]
    chips = lax.axis_size("tx")
    share = features // (chips * CORES)
    pair = lax.axis_index("pair") if paired else 0 * lax.axis_index("tc")
    where = jnp.stack([pair, lax.axis_index("tc")]).astype(jnp.int32)
    vmem = pl.BlockSpec(memory_space=pltpu.VMEM)
    return pl.pallas_call(
        mixer_body,
        in_specs=[pl.BlockSpec(memory_space=pltpu.SMEM), vmem, vmem, vmem, vmem, vmem],
        out_specs=[vmem, vmem],
        out_shape=[
            jax.ShapeDtypeStruct((chips, rows, share), jnp.float32),
            jax.ShapeDtypeStruct((chips, rows, share), jnp.bfloat16),
        ],
        compiler_params=pltpu.CompilerParams(vmem_limit_bytes=16 * 1024 * 1024),
        cost_estimate=pl.CostEstimate(
            flops=4 * rows * features * width,
            bytes_accessed=2 * features * (rows + 2 * width) + 6 * rows * features,
            transcendentals=0,
        ),
        name="mixer_terms",
    )(where, normed, product, taps, late_a, late_b)


def down_body(side, hidden, weights, out):
    chips, _, share = out.shape
    for chip in range(chips):
        piece = pl.ds(pl.multiple_of((CORES * chip + side[0]) * share, share), share)
        out[chip] = dot_t(hidden[...], weights[weights.shape[0] - 1, piece, :]).astype(out.dtype)


def down_terms(hidden, weights, side, dtype):
    rows, width = hidden.shape
    features = weights.shape[1]
    chips = lax.axis_size("tx")
    vmem = pl.BlockSpec(memory_space=pltpu.VMEM)
    return pl.pallas_call(
        down_body,
        in_specs=[pl.BlockSpec(memory_space=pltpu.SMEM), vmem, vmem],
        out_specs=vmem,
        out_shape=jax.ShapeDtypeStruct((chips, rows, features // (chips * CORES)), dtype),
        compiler_params=pltpu.CompilerParams(vmem_limit_bytes=24 * 1024 * 1024),
        cost_estimate=pl.CostEstimate(
            flops=rows * features * width,
            bytes_accessed=features * width + 3 * rows * features,
            transcendentals=0,
        ),
        name="down_terms",
    )(side.astype(jnp.int32).reshape(1), hidden, weights)


def on_device(
    tokens,
    mix_gain,
    w_signal,
    w_outer_gate,
    w_inner_gate,
    mix_taps,
    w_mix_out,
    ffn_gain,
    w_gate,
    w_value,
    up_taps,
    up_bias,
    w_down,
    paired,
):
    shards = jnp.stack((w_gate, w_value, w_down.T))
    ffn_full = lax.all_gather(shards, FS, axis=1, tiled=True)
    whole = gathered_copies(tokens, TP)
    early_a, early_b, late_a, late_b = mixer_weights(
        w_signal, w_outer_gate, w_inner_gate, w_mix_out.T, paired
    )
    normed = rms_norm(whole, mix_gain)
    product = rounded(dot(normed, early_a)) * rounded(dot(normed, early_b))
    mix_sum = pairs_and_summed(
        *mixer_terms(normed, product, mix_taps, late_a, late_b, paired)
    )
    resid = (tokens.astype(jnp.float32) + mix_sum).astype(jnp.bfloat16)
    whole_ffn = gathered_features(resid)
    normed_ffn = rms_norm(whole_ffn, ffn_gain)
    gate = rounded(dot(normed_ffn, ffn_full[0]))
    value = rounded(dot(normed_ffn, ffn_full[1]))
    gate_conv = conv_positions(gate, up_taps[0]) + up_bias[0]
    value_conv = conv_positions(value, up_taps[1]) + up_bias[1]
    hidden = (jax.nn.silu(gate_conv) * value_conv).astype(jnp.bfloat16)
    core = lax.axis_index("tc")
    send = down_terms(hidden, ffn_full, 1 - core, jnp.bfloat16)
    keep = down_terms(hidden, ffn_full, core, jnp.float32)
    ffn_sum = pairs_and_summed(keep, send)
    return (resid.astype(jnp.float32) + ffn_sum).astype(jnp.bfloat16)


def solution(mesh):
    groups, depth, wide = (mesh.shape[name] for name in ("grp", "fs", "tp"))
    pair = 2 if groups % 2 == 0 else 1
    split = Mesh(
        mesh.devices.reshape(
            groups // pair, pair, depth // NEAR, NEAR, wide // CORES, CORES
        ),
        ("gp", "pair", *FS, *TP),
    )
    streams = P(("gp", "pair", *FS), TP)
    placed = (
        streams,
        P(),
        P(FS, TP),
        P(FS, TP),
        P(FS, TP),
        P(None, TP),
        P(TP, FS),
        P(),
        P(FS, TP),
        P(FS, TP),
        P(None, None, TP),
        P(None, TP),
        P(TP, FS),
    )

    def body(*args):
        return on_device(*args, paired=pair == 2)

    return jax.shard_map(
        body, mesh=split, in_specs=placed, out_specs=streams, check_vma=False
    )
```

```python
import jax
import jax.numpy as jnp
from jax import lax
from jax.experimental import pallas as pl
from jax.experimental.pallas import tpu as pltpu
from jax.sharding import Mesh
from jax.sharding import PartitionSpec as P

SEQS_DEV = 2
CORES = 2
NEAR = 2

TP = ("tx", "tc")
FS = ("fa", "fb")


def side_by_side(arrays):
    return jnp.concatenate(arrays, axis=1)


def gathered_copies(value, axis):
    count = lax.axis_size(axis)
    copies = jnp.broadcast_to(value, (count, *value.shape))
    pieces = lax.all_to_all(copies, axis, split_axis=0, concat_axis=0, tiled=True)
    rows, width = value.shape
    return jnp.moveaxis(pieces, 0, 1).reshape(rows, count * width)


def swapped(value, axis):
    return lax.ppermute(value, axis, [(0, 1), (1, 0)])


def by_core(own, other):
    first = lax.axis_index("tc") == 0
    return jnp.where(first, own, other), jnp.where(first, other, own)


def gathered_features(value):
    own = lax.all_gather(value, "tx", axis=0)
    other = swapped(own, "tc")
    pieces = [piece for chip in range(own.shape[0]) for piece in by_core(own[chip], other[chip])]
    return jnp.concatenate(pieces, axis=1)


def pairs_and_summed(keep, send):
    received = swapped(send, "tc")
    pairs = (keep + received.astype(jnp.float32)).astype(jnp.bfloat16)
    parts = lax.all_to_all(pairs, "tx", 0, 0, tiled=True)
    return jnp.sum(parts.astype(jnp.float32), axis=0)


def conv_positions(values, taps):
    width = values.shape[1]
    blocks = values.reshape(SEQS_DEV, -1, width)
    length = blocks.shape[1]
    padded = jnp.pad(blocks, ((0, 0), (2, 0), (0, 0)))
    result = (
        padded[:, 0:length] * taps[0]
        + padded[:, 1 : length + 1] * taps[1]
        + padded[:, 2 : length + 2] * taps[2]
    )
    return result.reshape(-1, width)


def rms_norm(stream, gain):
    values = stream.astype(jnp.float32)
    scale = lax.rsqrt(jnp.mean(values * values, axis=-1, keepdims=True) + 1e-06)
    return (values * scale * gain).astype(jnp.bfloat16)


def dot(left, right):
    return jnp.dot(left, right, preferred_element_type=jnp.float32)


def dot_t(left, right_t):
    return lax.dot_general(
        left, right_t, (((1,), (1,)), ((), ())), preferred_element_type=jnp.float32
    )


def near_gather(far):
    wide = lax.all_gather(far, "fb", axis=1, tiled=True)
    return wide.reshape(-1, far.shape[-1])


def rounded(value):
    return value.astype(jnp.bfloat16).astype(jnp.float32)


def mixer_weights(w_signal, w_outer_gate, w_inner_gate, mix_out_t, paired):
    if not paired:
        shards = (w_signal, w_inner_gate, w_outer_gate, mix_out_t)
        far = lax.all_gather(side_by_side(shards), "fa", axis=0)
        width = w_signal.shape[1]
        return tuple(near_gather(far[:, :, k * width : (k + 1) * width]) for k in range(4))
    first = lax.axis_index("pair") == 0
    early = jnp.where(first, w_signal, w_inner_gate)
    late = jnp.where(first, w_outer_gate, mix_out_t)
    width = early.shape[1]
    far = lax.all_gather(side_by_side((early, late)), "fa", axis=0)
    early_own = near_gather(far[:, :, :width])
    early_other = swapped(early_own, "pair")
    late_own = near_gather(far[:, :, width:])
    late_other = swapped(late_own, "pair")
    return early_own, early_other, late_own, late_other


def mixer_body(where, normed, product, taps, late_a, late_b, keep, send):
    rows = normed.shape[0]
    chips, _, share = keep.shape
    first = where[0] == 0
    own = where[1]
    outer_full = jnp.where(first, late_a[...], late_b[...])
    outer = rounded(dot(normed[...], outer_full))
    values = product[...]
    place = lax.broadcasted_iota(jnp.int32, values.shape, 0) % (rows // SEQS_DEV)
    one = jnp.where(place >= 1, pltpu.roll(values, 1, 0), 0.0)
    two = jnp.where(place >= 2, pltpu.roll(values, 2, 0), 0.0)
    conv = two * taps[0:1, :] + one * taps[1:2, :] + values * taps[2:3, :]
    mixed = (outer * conv).astype(jnp.bfloat16)

    def terms(chip, side):
        piece = pl.ds(pl.multiple_of((CORES * chip + side) * share, share), share)
        return dot_t(mixed, jnp.where(first, late_b[piece, :], late_a[piece, :]))

    for chip in range(chips):
        send[chip] = terms(chip, 1 - own).astype(send.dtype)
    for chip in range(chips):
        keep[chip] = terms(chip, own)


def mixer_terms(normed, product, taps, late_a, late_b, paired):
    rows, features = normed.shape
    width = product.shape[1]
    chips = lax.axis_size("tx")
    share = features // (chips * CORES)
    pair = lax.axis_index("pair") if paired else 0 * lax.axis_index("tc")
    where = jnp.stack([pair, lax.axis_index("tc")]).astype(jnp.int32)
    vmem = pl.BlockSpec(memory_space=pltpu.VMEM)
    return pl.pallas_call(
        mixer_body,
        in_specs=[pl.BlockSpec(memory_space=pltpu.SMEM), vmem, vmem, vmem, vmem, vmem],
        out_specs=[vmem, vmem],
        out_shape=[
            jax.ShapeDtypeStruct((chips, rows, share), jnp.float32),
            jax.ShapeDtypeStruct((chips, rows, share), jnp.bfloat16),
        ],
        compiler_params=pltpu.CompilerParams(vmem_limit_bytes=16 * 1024 * 1024),
        cost_estimate=pl.CostEstimate(
            flops=4 * rows * features * width,
            bytes_accessed=2 * features * (rows + 2 * width) + 6 * rows * features,
            transcendentals=0,
        ),
        name="mixer_terms",
    )(where, normed, product, taps, late_a, late_b)


def down_body(side, hidden, weights, out):
    chips, _, share = out.shape
    for chip in range(chips):
        piece = pl.ds(pl.multiple_of((CORES * chip + side[0]) * share, share), share)
        out[chip] = dot_t(hidden[...], weights[weights.shape[0] - 1, piece, :]).astype(out.dtype)


def down_terms(hidden, weights, side, dtype):
    rows, width = hidden.shape
    features = weights.shape[1]
    chips = lax.axis_size("tx")
    vmem = pl.BlockSpec(memory_space=pltpu.VMEM)
    return pl.pallas_call(
        down_body,
        in_specs=[pl.BlockSpec(memory_space=pltpu.SMEM), vmem, vmem],
        out_specs=vmem,
        out_shape=jax.ShapeDtypeStruct((chips, rows, features // (chips * CORES)), dtype),
        compiler_params=pltpu.CompilerParams(vmem_limit_bytes=24 * 1024 * 1024),
        cost_estimate=pl.CostEstimate(
            flops=rows * features * width,
            bytes_accessed=features * width + 3 * rows * features,
            transcendentals=0,
        ),
        name="down_terms",
    )(side.astype(jnp.int32).reshape(1), hidden, weights)


def on_device(
    tokens,
    mix_gain,
    w_signal,
    w_outer_gate,
    w_inner_gate,
    mix_taps,
    w_mix_out,
    ffn_gain,
    w_gate,
    w_value,
    up_taps,
    up_bias,
    w_down,
    paired,
):
    shards = jnp.stack((w_gate, w_value, w_down.T))
    ffn_full = lax.all_gather(shards, FS, axis=1, tiled=True)
    whole = gathered_copies(tokens, TP)
    early_a, early_b, late_a, late_b = mixer_weights(
        w_signal, w_outer_gate, w_inner_gate, w_mix_out.T, paired
    )
    normed = rms_norm(whole, mix_gain)
    product = rounded(dot(normed, early_a)) * rounded(dot(normed, early_b))
    mix_sum = pairs_and_summed(
        *mixer_terms(normed, product, mix_taps, late_a, late_b, paired)
    )
    resid = (tokens.astype(jnp.float32) + mix_sum).astype(jnp.bfloat16)
    whole_ffn = gathered_features(resid)
    normed_ffn = rms_norm(whole_ffn, ffn_gain)
    gate = rounded(dot(normed_ffn, ffn_full[0]))
    value = rounded(dot(normed_ffn, ffn_full[1]))
    gate_conv = conv_positions(gate, up_taps[0]) + up_bias[0]
    value_conv = conv_positions(value, up_taps[1]) + up_bias[1]
    hidden = (jax.nn.silu(gate_conv) * value_conv).astype(jnp.bfloat16)
    core = lax.axis_index("tc")
    send = down_terms(hidden, ffn_full, 1 - core, jnp.bfloat16)
    keep = down_terms(hidden, ffn_full, core, jnp.float32)
    ffn_sum = pairs_and_summed(keep, send)
    return (resid.astype(jnp.float32) + ffn_sum).astype(jnp.bfloat16)


def solution(mesh):
    groups, depth, wide = (mesh.shape[name] for name in ("grp", "fs", "tp"))
    pair = 2 if groups % 2 == 0 else 1
    split = Mesh(
        mesh.devices.reshape(
            groups // pair, pair, depth // NEAR, NEAR, wide // CORES, CORES
        ),
        ("gp", "pair", *FS, *TP),
    )
    streams = P(("gp", "pair", *FS), TP)
    placed = (
        streams,
        P(),
        P(FS, TP),
        P(FS, TP),
        P(FS, TP),
        P(None, TP),
        P(TP, FS),
        P(),
        P(FS, TP),
        P(FS, TP),
        P(None, None, TP),
        P(None, TP),
        P(TP, FS),
    )

    def body(*args):
        return on_device(*args, paired=pair == 2)

    return jax.shard_map(
        body, mesh=split, in_specs=placed, out_specs=streams, check_vma=False
    )
```

```python
import jax
import jax.numpy as jnp
from jax import lax
from jax.experimental import pallas as pl
from jax.experimental.pallas import tpu as pltpu
from jax.sharding import Mesh
from jax.sharding import PartitionSpec as P

SEQS_DEV = 2
CORES = 2
NEAR = 2

TP = ("tx", "tc")
FS = ("fa", "fb")


def side_by_side(arrays):
    return jnp.concatenate(arrays, axis=1)


def gathered_copies(value, axis):
    count = lax.axis_size(axis)
    copies = jnp.broadcast_to(value, (count, *value.shape))
    pieces = lax.all_to_all(copies, axis, split_axis=0, concat_axis=0, tiled=True)
    rows, width = value.shape
    return jnp.moveaxis(pieces, 0, 1).reshape(rows, count * width)


def swapped(value, axis):
    return lax.ppermute(value, axis, [(0, 1), (1, 0)])


def by_core(own, other):
    first = lax.axis_index("tc") == 0
    return jnp.where(first, own, other), jnp.where(first, other, own)


def gathered_features(value):
    own = lax.all_gather(value, "tx", axis=0)
    other = swapped(own, "tc")
    pieces = [piece for chip in range(own.shape[0]) for piece in by_core(own[chip], other[chip])]
    return jnp.concatenate(pieces, axis=1)


def pairs_and_summed(keep, send):
    received = swapped(send, "tc")
    pairs = (keep + received.astype(jnp.float32)).astype(jnp.bfloat16)
    parts = lax.all_to_all(pairs, "tx", 0, 0, tiled=True)
    return jnp.sum(parts.astype(jnp.float32), axis=0)


def conv_positions(values, taps):
    width = values.shape[1]
    blocks = values.reshape(SEQS_DEV, -1, width)
    length = blocks.shape[1]
    padded = jnp.pad(blocks, ((0, 0), (2, 0), (0, 0)))
    result = (
        padded[:, 0:length] * taps[0]
        + padded[:, 1 : length + 1] * taps[1]
        + padded[:, 2 : length + 2] * taps[2]
    )
    return result.reshape(-1, width)


def rms_norm(stream, gain):
    values = stream.astype(jnp.float32)
    scale = lax.rsqrt(jnp.mean(values * values, axis=-1, keepdims=True) + 1e-06)
    return (values * scale * gain).astype(jnp.bfloat16)


def dot(left, right):
    return jnp.dot(left, right, preferred_element_type=jnp.float32)


def dot_t(left, right_t):
    return lax.dot_general(
        left, right_t, (((1,), (1,)), ((), ())), preferred_element_type=jnp.float32
    )


def near_gather(far):
    wide = lax.all_gather(far, "fb", axis=1, tiled=True)
    return wide.reshape(-1, far.shape[-1])


def rounded(value):
    return value.astype(jnp.bfloat16).astype(jnp.float32)


def mixer_weights(w_signal, w_outer_gate, w_inner_gate, mix_out_t, paired):
    if not paired:
        shards = (w_signal, w_inner_gate, w_outer_gate, mix_out_t)
        far = lax.all_gather(side_by_side(shards), "fa", axis=0)
        width = w_signal.shape[1]
        return tuple(near_gather(far[:, :, k * width : (k + 1) * width]) for k in range(4))
    first = lax.axis_index("pair") == 0
    early = jnp.where(first, w_signal, w_inner_gate)
    late = jnp.where(first, w_outer_gate, mix_out_t)
    width = early.shape[1]
    far = lax.all_gather(side_by_side((early, late)), "fa", axis=0)
    early_own = near_gather(far[:, :, :width])
    early_other = swapped(early_own, "pair")
    late_own = near_gather(far[:, :, width:])
    late_other = swapped(late_own, "pair")
    return early_own, early_other, late_own, late_other


def mixer_body(where, normed, product, taps, late_a, late_b, keep, send):
    rows = normed.shape[0]
    chips, _, share = keep.shape
    first = where[0] == 0
    own = where[1]
    outer_full = jnp.where(first, late_a[...], late_b[...])
    outer = rounded(dot(normed[...], outer_full))
    values = product[...]
    place = lax.broadcasted_iota(jnp.int32, values.shape, 0) % (rows // SEQS_DEV)
    one = jnp.where(place >= 1, pltpu.roll(values, 1, 0), 0.0)
    two = jnp.where(place >= 2, pltpu.roll(values, 2, 0), 0.0)
    conv = two * taps[0:1, :] + one * taps[1:2, :] + values * taps[2:3, :]
    mixed = (outer * conv).astype(jnp.bfloat16)

    def terms(chip, side):
        piece = pl.ds(pl.multiple_of((CORES * chip + side) * share, share), share)
        return dot_t(mixed, jnp.where(first, late_b[piece, :], late_a[piece, :]))

    for chip in range(chips):
        send[chip] = terms(chip, 1 - own).astype(send.dtype)
    for chip in range(chips):
        keep[chip] = terms(chip, own)


def mixer_terms(normed, product, taps, late_a, late_b, paired):
    rows, features = normed.shape
    width = product.shape[1]
    chips = lax.axis_size("tx")
    share = features // (chips * CORES)
    pair = lax.axis_index("pair") if paired else 0 * lax.axis_index("tc")
    where = jnp.stack([pair, lax.axis_index("tc")]).astype(jnp.int32)
    vmem = pl.BlockSpec(memory_space=pltpu.VMEM)
    return pl.pallas_call(
        mixer_body,
        in_specs=[pl.BlockSpec(memory_space=pltpu.SMEM), vmem, vmem, vmem, vmem, vmem],
        out_specs=[vmem, vmem],
        out_shape=[
            jax.ShapeDtypeStruct((chips, rows, share), jnp.float32),
            jax.ShapeDtypeStruct((chips, rows, share), jnp.bfloat16),
        ],
        compiler_params=pltpu.CompilerParams(vmem_limit_bytes=16 * 1024 * 1024),
        cost_estimate=pl.CostEstimate(
            flops=4 * rows * features * width,
            bytes_accessed=2 * features * (rows + 2 * width) + 6 * rows * features,
            transcendentals=0,
        ),
        name="mixer_terms",
    )(where, normed, product, taps, late_a, late_b)


def down_body(side, hidden, weights, out):
    chips, _, share = out.shape
    for chip in range(chips):
        piece = pl.ds(pl.multiple_of((CORES * chip + side[0]) * share, share), share)
        out[chip] = dot_t(hidden[...], weights[weights.shape[0] - 1, piece, :]).astype(out.dtype)


def down_terms(hidden, weights, side, dtype):
    rows, width = hidden.shape
    features = weights.shape[1]
    chips = lax.axis_size("tx")
    vmem = pl.BlockSpec(memory_space=pltpu.VMEM)
    return pl.pallas_call(
        down_body,
        in_specs=[pl.BlockSpec(memory_space=pltpu.SMEM), vmem, vmem],
        out_specs=vmem,
        out_shape=jax.ShapeDtypeStruct((chips, rows, features // (chips * CORES)), dtype),
        compiler_params=pltpu.CompilerParams(vmem_limit_bytes=24 * 1024 * 1024),
        cost_estimate=pl.CostEstimate(
            flops=rows * features * width,
            bytes_accessed=features * width + 3 * rows * features,
            transcendentals=0,
        ),
        name="down_terms",
    )(side.astype(jnp.int32).reshape(1), hidden, weights)


def on_device(
    tokens,
    mix_gain,
    w_signal,
    w_outer_gate,
    w_inner_gate,
    mix_taps,
    w_mix_out,
    ffn_gain,
    w_gate,
    w_value,
    up_taps,
    up_bias,
    w_down,
    paired,
):
    shards = jnp.stack((w_gate, w_value, w_down.T))
    ffn_full = lax.all_gather(shards, FS, axis=1, tiled=True)
    whole = gathered_copies(tokens, TP)
    early_a, early_b, late_a, late_b = mixer_weights(
        w_signal, w_outer_gate, w_inner_gate, w_mix_out.T, paired
    )
    normed = rms_norm(whole, mix_gain)
    product = rounded(dot(normed, early_a)) * rounded(dot(normed, early_b))
    mix_sum = pairs_and_summed(
        *mixer_terms(normed, product, mix_taps, late_a, late_b, paired)
    )
    resid = (tokens.astype(jnp.float32) + mix_sum).astype(jnp.bfloat16)
    whole_ffn = gathered_features(resid)
    normed_ffn = lax.optimization_barrier(rms_norm(whole_ffn, ffn_gain))
    gate = rounded(dot(normed_ffn, ffn_full[0]))
    value = rounded(dot(normed_ffn, ffn_full[1]))
    gate_conv = conv_positions(gate, up_taps[0]) + up_bias[0]
    value_conv = conv_positions(value, up_taps[1]) + up_bias[1]
    hidden = (jax.nn.silu(gate_conv) * value_conv).astype(jnp.bfloat16)
    core = lax.axis_index("tc")
    send = down_terms(hidden, ffn_full, 1 - core, jnp.bfloat16)
    keep = down_terms(hidden, ffn_full, core, jnp.float32)
    ffn_sum = pairs_and_summed(keep, send)
    return (resid.astype(jnp.float32) + ffn_sum).astype(jnp.bfloat16)


def solution(mesh):
    groups, depth, wide = (mesh.shape[name] for name in ("grp", "fs", "tp"))
    pair = 2 if groups % 2 == 0 else 1
    split = Mesh(
        mesh.devices.reshape(
            groups // pair, pair, depth // NEAR, NEAR, wide // CORES, CORES
        ),
        ("gp", "pair", *FS, *TP),
    )
    streams = P(("gp", "pair", *FS), TP)
    placed = (
        streams,
        P(),
        P(FS, TP),
        P(FS, TP),
        P(FS, TP),
        P(None, TP),
        P(TP, FS),
        P(),
        P(FS, TP),
        P(FS, TP),
        P(None, None, TP),
        P(None, TP),
        P(TP, FS),
    )

    def body(*args):
        return on_device(*args, paired=pair == 2)

    return jax.shard_map(
        body, mesh=split, in_specs=placed, out_specs=streams, check_vma=False
    )
```
